1024 devices in a mesh: ep: 64 (over z, core), tp: 16 (over y, x).
Axes of the slice: x: 4, y: 4, z: 32, core: 2. Of those that a mesh axis runs over, the one named last changes fastest.
Arguments:
- resid_in: bfloat16 [2048, 2048], P('ep'), may hold values from -10 to 10
- state_in: float32 [2048, 1024, 128], P('ep', 'tp'), may hold values from -6 to 6
- mix_gain: bfloat16 [2048], replicated, may hold values from 0.099609375 to 1.8984375
- query_weight: bfloat16 [2048, 512], replicated, may hold values from -0.125 to 0.125
- key_weight: bfloat16 [2048, 512], replicated, may hold values from -0.125 to 0.125
- decay_weight: bfloat16 [2048, 512], replicated, may hold values from -0.375 to 0.375
- value_weight: bfloat16 [2048, 1024], P(None, 'tp'), may hold values from -0.125 to 0.125
- decay_bias: float32 [512], replicated, may hold values from -12 to 4
- proj_weight: bfloat16 [1024, 2048], P('tp'), may hold values from -0.25 to 0.25
- ffn_gain: bfloat16 [2048], P('tp'), may hold values from 0.099609375 to 1.8984375
- expert_gate: bfloat16 [64, 2048, 256], P('ep', 'tp'), may hold values from -0.125 to 0.125
- expert_up: bfloat16 [64, 2048, 256], P('ep', 'tp'), may hold values from -0.125 to 0.125
- expert_down: bfloat16 [64, 256, 2048], P('ep', None, 'tp'), may hold values from -0.375 to 0.375
- route_group: int32 [2048], replicated, may hold values from 0 to 15, as said below
- route_pick: int32 [2048, 2], replicated, may hold values from 0 to 3, as said below
- route_weight: float32 [2048, 2], replicated, may hold values from 0.2 to 1
Outputs:
- resid_out: bfloat16 [2048, 2048], P('ep', 'tp')
- state_out: float32 [2048, 1024, 128], P('ep', 'tp')
The draws below stay inside these ranges and needn't reach their ends.
Inputs may be any that keep to these rules, and one draw needn't show every extreme that they name: `route_group`: group g holds experts 4 * g to 4 * g + 3. Among the 32 tokens of one aligned block, no expert is named by more than 2 pairs (token, k), and in every draw some expert is named by exactly 2 pairs in every block. `route_pick`: the 2 entries of a token differ.
All inputs are finite; a program needn't handle non-finite values.
Results may differ from the reference program's by a relative error of at most 0.015.
Values may be sent and summed in bfloat16 or wider, within the bound.
A program may use at most 64 MiB of HBM per device.

```python
import math
import jax
import jax.numpy as jnp
from jax import lax

D = 2048
HEADS = 4
DK = 128
DV = 256
FF = 256
EPG = 4
TOPK = 2
SEQ_DEV = 32
EXPERTS = 64
GROUPS = 16
CAP = 2
TOKENS = 2048
N_EP = 64
N_TP = 16


def inner_order(one_key):
    return jax.random.permutation(one_key, EPG)


def routing_tables(key):
    base_key = jax.random.fold_in(key, 23)
    per_group = EPG * CAP // 2
    slot_total = GROUPS * per_group
    order_key, hot_key, block_key = jax.random.split(base_key, 3)
    favoured = jax.random.permutation(order_key, GROUPS)
    hottest = jax.random.randint(hot_key, (), 0, GROUPS)
    slot_group = jnp.arange(slot_total, dtype=jnp.int32) // per_group

    def one_block(block_seed):
        subkeys = jax.random.split(block_seed, 5)
        first_draw = jax.random.randint(subkeys[0], (), 0, GROUPS)
        second_draw = jax.random.randint(subkeys[1], (), 0, GROUPS)
        filled = favoured[jnp.minimum(first_draw, second_draw)]
        shuffled = jax.random.permutation(subkeys[2], slot_total).astype(jnp.int32)
        scores = jnp.where((slot_group == filled) | (slot_group == hottest), 0, 1 + shuffled)
        chosen = jnp.argsort(scores, stable=True)[:SEQ_DEV]
        chosen = jax.random.permutation(subkeys[3], chosen)
        group_of = chosen // per_group
        within = chosen % per_group
        orders = jax.vmap(inner_order)(jax.random.split(subkeys[4], GROUPS))
        first_pick = orders[group_of, 2 * within % EPG]
        second_pick = orders[group_of, (2 * within + 1) % EPG]
        return (group_of, jnp.stack([first_pick, second_pick], axis=1))
    groups, pick_pairs = jax.vmap(one_block)(jax.random.split(block_key, N_EP))
    return (groups.reshape(TOKENS).astype(jnp.int32), pick_pairs.reshape(TOKENS, TOPK).astype(jnp.int32))


def draw_route_group(key, part):
    return routing_tables(key)[0]


def draw_route_pick(key, part):
    return routing_tables(key)[1]


def draw_resid_in(key, part):
    base_key, rough_key = jax.random.split(jax.random.fold_in(key, 5))
    column = jnp.arange(D, dtype=jnp.float32) / D
    rough = jax.random.uniform(rough_key, (D,), jnp.float32, 0.6, 1.4)
    values = jnp.clip(jax.random.normal(base_key, (TOKENS, D), jnp.float32), -3.5, 3.5)
    scale = jnp.exp(jnp.log(3.0) * column) * 0.6
    return (values * scale[None, :] * rough[None, :]).astype(jnp.bfloat16)


def spiked(entries, own_key, source, target, blocks, factor):
    owner, partner = [(jnp.arange(entries.shape[axis_at]) // (entries.shape[axis_at] // blocks)).reshape([-1 if axis == axis_at else 1 for axis in range(entries.ndim)]) for axis_at in (source, target)]
    chosen = jax.random.permutation(own_key, blocks)[partner]
    strong = (owner == chosen) | (owner == (partner + blocks // 2) % blocks)
    return jnp.where(strong, factor * entries, entries)


def block_scale(rng, dims, cuts, least, high):
    gain, own = 1.0, jax.random.fold_in(rng, 6)
    for dim, parts in cuts:
        draws = jnp.exp(jax.random.uniform(jax.random.fold_in(own, dim), (parts,), jnp.float32, least / len(cuts), high / len(cuts)))
        gain = gain * jnp.repeat(draws, dims[dim] // parts).reshape([-1 if axis == dim else 1 for axis in range(len(dims))])
    return gain


def noise(rng, dims, deviation, reach, cuts=(), held_as=jnp.bfloat16):
    drawn = jax.random.normal(rng, dims, jnp.float32) * deviation
    if len(cuts) > 0:
        drawn = block_scale(rng, dims, cuts, -0.22, 0.18) * drawn
    return jnp.clip(drawn, min=-reach, max=reach).astype(held_as)


def bell_draw_with(key, extent, spread, bound, cuts, heavy, held_as=jnp.bfloat16):
    values = spread * jax.random.normal(key, extent, jnp.float32)
    if cuts:
        values = values * block_scale(key, extent, cuts, -0.22, 0.18)
    return jnp.clip(spiked(values, jax.random.fold_in(key, 3), *heavy), -bound, bound).astype(held_as)


def setup_inputs(seed: int = 0) -> dict:
    splits = jax.random.split(jax.random.key(seed), 17)
    resid_in = draw_resid_in(jax.random.fold_in(splits[16], 71), 0)
    state_in = noise(splits[1], (TOKENS, HEADS * DV, DK), 1.0, 6.0, ((0, 64), (1, 16)), jnp.float32)
    mix_gain = jnp.clip(1.0 + 0.18 * jax.random.normal(splits[2], (D,), jnp.float32), 0.099609375, 1.8984375).astype(jnp.bfloat16)
    query_weight = noise(splits[3], (D, HEADS * DK), D ** -0.5, 0.125)
    key_weight = noise(splits[4], (D, HEADS * DK), D ** -0.5, 0.125)
    decay_weight = noise(splits[5], (D, HEADS * DK), (D // 9) ** -0.5, 0.375)
    value_weight = noise(splits[6], (D, HEADS * DV), D ** -0.5, 0.125, ((1, 16),))
    decay_bias = jnp.clip(jax.random.uniform(splits[7], (HEADS * DK,), jnp.float32, -12.0, 4.0), -12.0, 4.0)
    proj_weight = bell_draw_with(splits[8], (HEADS * DV, D), (HEADS * DV) ** -0.5, 0.25, ((0, 16),), (0, 1, 16, 2.0))
    ffn_gain = jnp.clip(1.0 + 0.18 * jax.random.normal(splits[9], (D,), jnp.float32), 0.099609375, 1.8984375).astype(jnp.bfloat16)
    expert_gate = noise(splits[10], (EXPERTS, D, FF), D ** -0.5, 0.125, ((0, 64), (1, 16)))
    expert_up = noise(splits[11], (EXPERTS, D, FF), D ** -0.5, 0.125, ((0, 64), (1, 16)))
    expert_down = noise(splits[12], (EXPERTS, FF, D), FF ** -0.5, 0.375, ((0, 64), (2, 16)))
    route_group = draw_route_group(jax.random.fold_in(splits[16], 71), 0)
    route_pick = draw_route_pick(jax.random.fold_in(splits[16], 71), 0)
    route_weight = jnp.clip(jnp.exp(jax.random.uniform(splits[15], (TOKENS, TOPK), jnp.float32, math.log(0.2), math.log(1.0))), 0.2, 1.0)
    return {"resid_in": resid_in, "state_in": state_in, "mix_gain": mix_gain, "query_weight": query_weight, "key_weight": key_weight, "decay_weight": decay_weight, "value_weight": value_weight, "decay_bias": decay_bias, "proj_weight": proj_weight, "ffn_gain": ffn_gain, "expert_gate": expert_gate, "expert_up": expert_up, "expert_down": expert_down, "route_group": route_group, "route_pick": route_pick, "route_weight": route_weight}


epsilon = 1e-06
gate_tau = 16.0

def inverse_rms(values):
    return lax.rsqrt(lax.optimization_barrier(jnp.mean(values * values, axis=-1, keepdims=True)) + epsilon)

def pair_slots(expert_ids, expert_count):
    onehot = (expert_ids[..., None] == jnp.arange(expert_count, dtype=jnp.int32)).astype(jnp.int32)
    earlier = jnp.cumsum(onehot, axis=-2) - onehot
    return lax.optimization_barrier(jnp.sum(earlier * onehot, axis=-1)).astype(jnp.int32)

def reference(resid_in, state_in, mix_gain, query_weight, key_weight, decay_weight, value_weight, decay_bias, proj_weight, ffn_gain, expert_gate, expert_up, expert_down, route_group, route_pick, route_weight):
    row_values = resid_in.astype(jnp.float32)
    normed_in = (row_values * inverse_rms(row_values) * mix_gain.astype(jnp.float32)).astype(jnp.bfloat16)
    queries = (jnp.dot(normed_in, query_weight, preferred_element_type=jnp.float32) * DK ** (-0.5)).astype(jnp.bfloat16)
    key_rows = jnp.dot(normed_in, key_weight, preferred_element_type=jnp.float32).astype(jnp.bfloat16)
    decay_rows = jnp.dot(normed_in, decay_weight, preferred_element_type=jnp.float32).astype(jnp.bfloat16)
    value_rows = jnp.dot(normed_in, value_weight, preferred_element_type=jnp.float32).astype(jnp.bfloat16)
    queries, key_rows, decay_rows, value_rows = lax.optimization_barrier((queries, key_rows, decay_rows, value_rows))
    forget = jnp.exp(jax.nn.log_sigmoid(decay_rows.astype(jnp.float32) + decay_bias[None, :]) / gate_tau)

    def one_block(block_item):
        state_part, forget_part, key_part, value_part, query_part = block_item
        state_new = forget_part[:, :, None, :] * state_part + value_part[:, :, :, None] * key_part[:, :, None, :]
        readout = jnp.einsum('thvk,thk->thv', state_new, query_part, precision=lax.Precision.HIGHEST)
        return (state_new, readout)
    state_blocks, read_blocks = lax.map(one_block, (state_in.reshape(N_EP, SEQ_DEV, HEADS, DV, DK), forget.reshape(N_EP, SEQ_DEV, HEADS, DK), key_rows.astype(jnp.float32).reshape(N_EP, SEQ_DEV, HEADS, DK), value_rows.astype(jnp.float32).reshape(N_EP, SEQ_DEV, HEADS, DV), queries.astype(jnp.float32).reshape(N_EP, SEQ_DEV, HEADS, DK)))
    state_out = state_blocks.reshape(TOKENS, HEADS * DV, DK)
    readout = read_blocks.reshape(TOKENS, HEADS * DV).astype(jnp.bfloat16)
    readout = lax.optimization_barrier(readout)
    block_width = HEADS * DV // N_TP
    head_part = jnp.einsum('tns,nsd->ntd', readout.astype(jnp.float32).reshape(TOKENS, N_TP, block_width), proj_weight.astype(jnp.float32).reshape(N_TP, block_width, D)).astype(jnp.bfloat16)
    head_part = lax.optimization_barrier(head_part)
    attention = lax.optimization_barrier(jnp.sum(head_part.astype(jnp.float32), axis=0)).astype(jnp.bfloat16)
    attention = lax.optimization_barrier(attention)
    middle = (row_values + attention.astype(jnp.float32)).astype(jnp.bfloat16)
    middle = lax.optimization_barrier(middle)
    middle_wide = middle.astype(jnp.float32)
    expert_in = (middle_wide * inverse_rms(middle_wide) * ffn_gain.astype(jnp.float32)).astype(jnp.bfloat16)
    expert_ids = EPG * route_group[:, None] + route_pick
    slot_of = pair_slots(expert_ids.reshape(N_EP, TOPK * SEQ_DEV), EXPERTS).reshape(TOKENS, TOPK)
    slot_rows = N_EP * CAP
    block_of = (jnp.arange(TOKENS, dtype=jnp.int32) // SEQ_DEV)[:, None]
    places = (expert_ids * slot_rows + block_of * CAP + slot_of).astype(jnp.int32)
    buffer = jnp.zeros((EXPERTS * slot_rows, D), jnp.bfloat16).at[places.reshape(-1)].set(jnp.repeat(expert_in, TOPK, axis=0))

    def run_expert(expert_item):
        inputs, gate_matrix, up_matrix, down_matrix = expert_item
        pieces = inputs.astype(jnp.float32).reshape(slot_rows, N_TP, D // N_TP)
        gate_parts = jnp.einsum('rnd,ndf->nrf', pieces, gate_matrix.astype(jnp.float32).reshape(N_TP, D // N_TP, FF)).astype(jnp.bfloat16)
        up_parts = jnp.einsum('rnd,ndf->nrf', pieces, up_matrix.astype(jnp.float32).reshape(N_TP, D // N_TP, FF)).astype(jnp.bfloat16)
        gate_parts, up_parts = lax.optimization_barrier((gate_parts, up_parts))
        gate_sum = lax.optimization_barrier(jnp.sum(gate_parts.astype(jnp.float32), axis=0))
        up_sum = lax.optimization_barrier(jnp.sum(up_parts.astype(jnp.float32), axis=0))
        active = (jax.nn.silu(gate_sum) * up_sum).astype(jnp.bfloat16)
        return jnp.dot(active, down_matrix, preferred_element_type=jnp.float32).astype(jnp.bfloat16)
    served = lax.map(run_expert, (buffer.reshape(EXPERTS, slot_rows, D), expert_gate, expert_up, expert_down))
    served = lax.optimization_barrier(served)
    picked = served.reshape(EXPERTS * slot_rows, D)[places].astype(jnp.float32)
    mixture = route_weight[:, 0:1] * picked[:, 0] + route_weight[:, 1:2] * picked[:, 1]
    resid_out = (middle_wide + mixture).astype(jnp.bfloat16)
    return (resid_out, state_out)
```

```python
import functools

import jax
import jax.numpy as jnp
from jax import lax
from jax.experimental import pallas as pl
from jax.experimental.pallas import tpu as pltpu
from jax.sharding import PartitionSpec as P

MESH = pl.DeviceIdType.MESH
F32 = jnp.float32
BF16 = jnp.bfloat16

epsilon = 1e-06
gate_tau = 16.0

SEQ = 32
WIDTH = 2048
DK = 128
DV = 256
VC = 64
PART = 128
FF = 256
CHIPS = 32
EXPERTS = 64
SIDE = 4
TPN = 16
NEAR = 4


def plane_offsets():
    steps = [(a, b) for a in range(SIDE) for b in range(SIDE) if a or b]
    return sorted(steps, key=lambda s: -(min(s[0], SIDE - s[0]) + min(s[1], SIDE - s[1])))


def line_offsets():
    return sorted(range(CHIPS), key=lambda s: -min(s, CHIPS - s))


def dot(a, b, dims=((1,), (0,))):
    return lax.dot_general(a, b, (dims, ((), ())), preferred_element_type=F32)


def layer_kernel(
    resid,
    state_in,
    mix_gain,
    query_w,
    key_w,
    decay_w,
    value_w,
    decay_bias,
    proj_w,
    ffn_gain,
    gate_w,
    up_w,
    down_w,
    group,
    pick,
    weight,
    resid_out,
    state_out,
    resid_v,
    mix_v,
    wq,
    wk,
    wd,
    wv,
    bias_v,
    wp,
    gain_v,
    wg,
    wu,
    wo,
    group_v,
    pick_v,
    weight_v,
    state_v,
    cols,
    part_s,
    part_r,
    rows_s,
    rows_r,
    hid_s,
    hid_r,
    act_s,
    act_r,
    back_s,
    back_r,
    out_v,
    load_sem,
    store_sem,
    send_sem,
    recv_sem,
    near_sem,
):
    ep = lax.axis_index("ep")
    tp = lax.axis_index("tp")
    z = ep // 2
    core = lax.rem(ep, 2)
    y = tp // SIDE
    x = lax.rem(tp, SIDE)
    head = tp // (DV // VC)
    block = ep // (PART // SEQ)
    head_cols = pl.ds(pl.multiple_of(head * DK, DK), DK)
    block_cols = pl.ds(pl.multiple_of(block * PART, PART), PART)

    pairs = [
        (resid, resid_v),
        (mix_gain, mix_v),
        (query_w.at[:, head_cols], wq),
        (key_w.at[:, head_cols], wk),
        (decay_w.at[:, head_cols], wd),
        (value_w, wv),
        (decay_bias, bias_v),
        (state_in, state_v),
        (proj_w, wp),
        (ffn_gain, gain_v),
        (group, group_v),
        (pick.at[:, block_cols], pick_v),
        (weight.at[:, block_cols], weight_v),
        (gate_w.at[0], wg),
        (up_w.at[0], wu),
        (down_w.at[0], wo),
    ]
    loads = [pltpu.make_async_copy(a, b, load_sem.at[i]) for i, (a, b) in enumerate(pairs)]

    for copy in loads:
        copy.start()

    def line_peer(step, other=0):
        return {"ep": lax.rem(z + step + CHIPS, CHIPS) * 2 + lax.rem(core + other, 2)}

    plane = [
        lax.rem(y + a, SIDE) * SIDE + lax.rem(x + b, SIDE) for a, b in plane_offsets()
    ]
    barrier = pltpu.get_barrier_semaphore()
    near = [{"tp": j} for j in plane] + [line_peer(0, 1)]
    for step in range(NEAR, 0, -1):
        for other in (0, 1):
            near += [line_peer(step, other), line_peer(-step, other)]
    for peer in near:
        pl.semaphore_signal(barrier, inc=1, device_id=peer, device_id_type=MESH)

    def ready(*which):
        for i in which:
            loads[i].wait()

    ready(0, 1)
    values = resid_v[...].astype(F32)
    inverse = lax.rsqrt(jnp.mean(values * values, axis=-1, keepdims=True) + epsilon)
    mix = mix_v[...].astype(F32)
    normed = jnp.concatenate(
        [
            (values[:, j * 128 : (j + 1) * 128] * inverse * mix[j : j + 1, :]).astype(BF16)
            for j in range(WIDTH // 128)
        ],
        axis=1,
    )

    pl.semaphore_wait(barrier, len(near))
    for step in (NEAR, -NEAR):
        pl.semaphore_signal(near_sem.at[0], inc=1, device_id=line_peer(step), device_id_type=MESH)

    ready(2, 3, 4, 5, 6)
    queries = (dot(normed, wq[...]) * DK ** (-0.5)).astype(BF16).astype(F32)
    keys = dot(normed, wk[...]).astype(BF16).astype(F32)
    decay = dot(normed, wd[...]).astype(BF16).astype(F32)
    value_t = dot(wv[...], normed, ((1,), (1,))).astype(BF16).astype(F32)
    logit = decay + bias_v[pl.ds(head, 1), :]
    log_gate = jnp.minimum(logit, 0.0) - jnp.log(1.0 + jnp.exp(-jnp.abs(logit)))
    forget = jnp.exp(log_gate / gate_tau)

    ready(7)
    lane = lax.broadcasted_iota(jnp.int32, (VC, SEQ), 1)
    readout_t = jnp.zeros((VC, SEQ), F32)
    for t in range(SEQ):
        new = (
            forget[t : t + 1, :] * state_v[t]
            + value_t[:, t : t + 1] * keys[t : t + 1, :]
        )
        state_v[t] = new
        total = jnp.sum(new * queries[t : t + 1, :], axis=1, keepdims=True)
        readout_t = jnp.where(lane == t, total, readout_t)
    store = pltpu.make_async_copy(state_v, state_out, store_sem.at[0])
    store.start()

    ready(8)
    partial = dot(readout_t.astype(BF16), wp[...], ((0,), (0,)))
    for j in range(TPN):
        part_s[j] = partial[:, j * PART : (j + 1) * PART].astype(BF16)

    pl.semaphore_wait(near_sem.at[0], 2)
    for step in (2 * NEAR, -2 * NEAR):
        pl.semaphore_signal(near_sem.at[1], inc=1, device_id=line_peer(step), device_id_type=MESH)

    def send(src, dst, phase, peer):
        pltpu.make_async_remote_copy(
            src_ref=src,
            dst_ref=dst,
            send_sem=send_sem.at[phase],
            recv_sem=recv_sem.at[phase],
            device_id=peer,
            device_id_type=MESH,
        ).start()

    def settle(ref, sem, phase):
        rest = ref.at[pl.ds(0, ref.shape[0] - 1)]
        pltpu.make_async_copy(rest, rest, sem.at[phase]).wait()

    for j in plane:
        send(part_s.at[j], part_r.at[tp], 0, {"tp": j})
    part_r[pl.ds(tp, 1)] = part_s[pl.ds(tp, 1)]

    ready(9, 10, 11, 12)
    base = group_v[pl.ds(block, 1), :] * 4
    first = (base + pick_v[0:1, :]).astype(F32)
    second = (base + pick_v[1:2, :]).astype(F32)
    sub = lax.broadcasted_iota(jnp.int32, (8, PART), 0)
    packed = jnp.where(
        sub == 0,
        first,
        jnp.where(sub == 1, second, jnp.where(sub == 2, weight_v[0:1, :], weight_v[1:2, :])),
    )
    cols[...] = packed.T
    own = cols[pl.ds(pl.multiple_of(lax.rem(ep, PART // SEQ) * SEQ, SEQ), SEQ), :]
    lanes = lax.broadcasted_iota(jnp.int32, (SEQ, 2 * EXPERTS), 1)
    expert_lane = (lanes // 2).astype(F32)
    slot_lane = lax.rem(lanes, 2).astype(F32)
    pick_a = (own[:, 0:1] == expert_lane).astype(F32)
    pick_b = (own[:, 1:2] == expert_lane).astype(F32)
    below = (
        lax.broadcasted_iota(jnp.int32, (SEQ, SEQ), 1)
        < lax.broadcasted_iota(jnp.int32, (SEQ, SEQ), 0)
    ).astype(F32)
    both = pick_a + pick_b
    earlier = dot(below.astype(BF16), both.astype(BF16))
    here = (earlier == slot_lane).astype(F32)
    select = (both * here).astype(BF16)
    mixing = (own[:, 2:3] * pick_a + own[:, 3:4] * pick_b) * here
    mixing_hi = mixing.astype(BF16)
    mixing_lo = (mixing - mixing_hi.astype(F32)).astype(BF16)
    select_t = select.astype(F32).T.astype(BF16)
    own_rows = resid_v[:, pl.ds(pl.multiple_of(tp * PART, PART), PART)].astype(F32)

    settle(part_r, recv_sem, 0)
    attention = jnp.sum(part_r[...].astype(F32), axis=0).astype(BF16)
    middle = (own_rows + attention.astype(F32)).astype(BF16)

    rows_s.reshape(2 * EXPERTS, PART)[...] = dot(select_t, middle).astype(BF16)
    pl.semaphore_wait(near_sem.at[1], 2)

    def to_line(src, dst, phase):
        for step in line_offsets():
            for other in (0, 1):
                if step == 0 and other == 0:
                    continue
                there = line_peer(step, other)
                send(src.at[there["ep"]], dst.at[ep], phase, there)
        dst[pl.ds(ep, 1)] = src[pl.ds(ep, 1)]

    to_line(rows_s, rows_r, 1)
    ready(13, 14, 15)
    gain = gain_v[...].astype(F32)
    settle(rows_r, recv_sem, 1)
    rows = rows_r.reshape(2 * EXPERTS, PART)[...].astype(F32)
    squares = jnp.sum(rows * rows, axis=1, keepdims=True)
    squares = jnp.broadcast_to(squares, (2 * EXPERTS, 128))
    squares_hi = squares.astype(BF16).astype(F32)
    squares_lo = squares - squares_hi
    scaled = (rows * gain).astype(BF16)
    gate_part = dot(scaled, wg[...])
    up_part = dot(scaled, wu[...])

    def owners(top, bottom):
        shape = (TPN, 8, top.shape[1])
        return jnp.concatenate([top.reshape(shape), bottom.reshape(shape)], axis=1).astype(BF16)

    hid_s[:, :, 0:FF] = owners(gate_part, up_part)
    hid_s[:, :, FF : FF + 128] = owners(squares_hi, squares_lo)
    for j in plane:
        send(hid_s.at[j], hid_r.at[tp], 2, {"tp": j})
    hid_r[pl.ds(tp, 1)] = hid_s[pl.ds(tp, 1)]
    settle(hid_r, recv_sem, 2)
    total = jnp.sum(hid_r[...].astype(F32), axis=0)
    square_sum = total[0:8, FF : FF + 128] + total[8:16, FF : FF + 128]
    scale = lax.rsqrt(square_sum / WIDTH + epsilon)
    scale = jnp.concatenate([scale, scale], axis=1)
    gate_pre = total[0:8, 0:FF] * scale
    up_pre = total[8:16, 0:FF] * scale
    active = gate_pre / (1.0 + jnp.exp(-gate_pre)) * up_pre
    act_s[...] = jnp.concatenate([active[:, 0:128], active[:, 128:256]], axis=0).astype(BF16)

    for j in plane:
        send(act_s, act_r.at[tp], 3, {"tp": j})
    act_r[pl.ds(tp, 1)] = act_s[...].reshape(1, 16, 128)
    settle(act_r, recv_sem, 3)
    acts = act_r[...].astype(F32)
    low = acts[:, 0:8, :].reshape(128, 128).astype(BF16)
    high = acts[:, 8:16, :].reshape(128, 128).astype(BF16)
    served = dot(low, wo[0:128, :]) + dot(high, wo[128:256, :])

    back_s.reshape(2 * EXPERTS, PART)[...] = served.astype(BF16)
    to_line(back_s, back_r, 4)
    settle(back_r, recv_sem, 4)
    back = back_r.reshape(2 * EXPERTS, PART)[...]
    mixture = dot(mixing_hi, back) + dot(mixing_lo, back)
    out_v[...] = (middle.astype(F32) + mixture).astype(BF16)
    last = pltpu.make_async_copy(out_v, resid_out, store_sem.at[1])
    last.start()

    settle(part_s, send_sem, 0)
    settle(rows_s, send_sem, 1)
    settle(hid_s, send_sem, 2)
    settle(act_r, send_sem, 3)
    settle(back_s, send_sem, 4)
    store.wait()
    last.wait()


def on_device(
    resid_in,
    state_in,
    mix_gain,
    query_weight,
    key_weight,
    decay_weight,
    value_weight,
    decay_bias,
    proj_weight,
    ffn_gain,
    expert_gate,
    expert_up,
    expert_down,
    route_group,
    route_pick,
    route_weight,
):
    args = (
        resid_in,
        state_in,
        mix_gain.reshape(WIDTH // 128, 128),
        query_weight,
        key_weight,
        decay_weight,
        value_weight.T,
        decay_bias.reshape(-1, DK),
        proj_weight,
        ffn_gain.reshape(1, PART),
        expert_gate,
        expert_up,
        expert_down,
        route_group.reshape(-1, 128),
        route_pick.T,
        route_weight.T,
    )
    vmem = pltpu.VMEM
    return pl.pallas_call(
        layer_kernel,
        out_shape=(
            jax.ShapeDtypeStruct((SEQ, PART), BF16),
            jax.ShapeDtypeStruct((SEQ, VC, DK), F32),
        ),
        in_specs=[pl.BlockSpec(memory_space=pl.ANY)] * len(args),
        out_specs=[pl.BlockSpec(memory_space=pl.ANY)] * 2,
        scratch_shapes=[
            vmem((SEQ, WIDTH), BF16),
            vmem((WIDTH // 128, 128), BF16),
            vmem((WIDTH, DK), BF16),
            vmem((WIDTH, DK), BF16),
            vmem((WIDTH, DK), BF16),
            vmem((VC, WIDTH), BF16),
            vmem((4, DK), F32),
            vmem((VC, WIDTH), BF16),
            vmem((1, PART), BF16),
            vmem((PART, FF), BF16),
            vmem((PART, FF), BF16),
            vmem((FF, PART), BF16),
            vmem((16, 128), jnp.int32),
            vmem((2, PART), jnp.int32),
            vmem((2, PART), F32),
            vmem((SEQ, VC, DK), F32),
            vmem((PART, 8), F32),
            vmem((TPN, SEQ, PART), BF16),
            vmem((TPN, SEQ, PART), BF16),
            vmem((EXPERTS, 2, PART), BF16),
            vmem((EXPERTS, 2, PART), BF16),
            vmem((TPN, 16, FF + 128), BF16),
            vmem((TPN, 16, FF + 128), BF16),
            vmem((16, 128), BF16),
            vmem((TPN, 16, 128), BF16),
            vmem((EXPERTS, 2, PART), BF16),
            vmem((EXPERTS, 2, PART), BF16),
            vmem((SEQ, PART), BF16),
            pltpu.SemaphoreType.DMA((16,)),
            pltpu.SemaphoreType.DMA((2,)),
            pltpu.SemaphoreType.DMA((5,)),
            pltpu.SemaphoreType.DMA((5,)),
            pltpu.SemaphoreType.REGULAR((2,)),
        ],
        compiler_params=pltpu.CompilerParams(collective_id=0, has_side_effects=True),
    )(*args)


def solution(mesh):
    return jax.shard_map(
        on_device,
        mesh=mesh,
        in_specs=(
            P("ep", None),
            P("ep", "tp", None),
            P(),
            P(),
            P(),
            P(),
            P(None, "tp"),
            P(),
            P("tp", None),
            P("tp"),
            P("ep", "tp", None),
            P("ep", "tp", None),
            P("ep", None, "tp"),
            P(),
            P(),
            P(),
        ),
        out_specs=(P("ep", "tp"), P("ep", "tp", None)),
        check_vma=False,
    )
```

```python
import functools

import jax
import jax.numpy as jnp
from jax import lax
from jax.experimental import pallas as pl
from jax.experimental.pallas import tpu as pltpu
from jax.sharding import PartitionSpec as P

MESH = pl.DeviceIdType.MESH
F32 = jnp.float32
BF16 = jnp.bfloat16

epsilon = 1e-06
gate_tau = 16.0

SEQ = 32
WIDTH = 2048
DK = 128
DV = 256
VC = 64
PART = 128
FF = 256
CHIPS = 32
EXPERTS = 64
SIDE = 4
TPN = 16
NEAR = 8


def plane_offsets():
    steps = [(a, b) for a in range(SIDE) for b in range(SIDE) if a or b]
    return sorted(steps, key=lambda s: -(min(s[0], SIDE - s[0]) + min(s[1], SIDE - s[1])))


def line_offsets():
    return sorted(range(CHIPS), key=lambda s: -min(s, CHIPS - s))


def dot(a, b, dims=((1,), (0,))):
    return lax.dot_general(a, b, (dims, ((), ())), preferred_element_type=F32)


def layer_kernel(
    resid,
    state_in,
    mix_gain,
    query_w,
    key_w,
    decay_w,
    value_w,
    decay_bias,
    proj_w,
    ffn_gain,
    gate_w,
    up_w,
    down_w,
    group,
    pick,
    weight,
    middle_out,
    mixing_out,
    back_out,
    state_out,
    resid_v,
    mix_v,
    wq,
    wk,
    wd,
    wv,
    bias_v,
    wp,
    gain_v,
    wg,
    wu,
    wo,
    group_v,
    pick_v,
    weight_v,
    state_v,
    cols,
    part_s,
    part_r,
    rows_s,
    rows_r,
    hid_s,
    hid_r,
    act_s,
    act_r,
    back_s,
    back_r,
    load_sem,
    send_sem,
    recv_sem,
    near_sem,
):
    ep = lax.axis_index("ep")
    tp = lax.axis_index("tp")
    z = ep // 2
    core = lax.rem(ep, 2)
    y = tp // SIDE
    x = lax.rem(tp, SIDE)
    head = tp // (DV // VC)
    block = ep // (PART // SEQ)
    head_cols = pl.ds(pl.multiple_of(head * DK, DK), DK)
    block_cols = pl.ds(pl.multiple_of(block * PART, PART), PART)

    pairs = [
        (resid, resid_v),
        (mix_gain, mix_v),
        (query_w.at[:, head_cols], wq),
        (key_w.at[:, head_cols], wk),
        (decay_w.at[:, head_cols], wd),
        (value_w, wv),
        (decay_bias, bias_v),
        (state_in, state_v),
        (proj_w, wp.at[pl.ds(0, VC)]),
        (ffn_gain, gain_v),
        (group, group_v),
        (pick.at[:, block_cols], pick_v),
        (weight.at[:, block_cols], weight_v),
        (gate_w.at[0], wg),
        (up_w.at[0], wu),
        (down_w.at[0], wo),
        (proj_w, wp.at[pl.ds(VC, VC)]),
    ]
    loads = [pltpu.make_async_copy(a, b, load_sem.at[i]) for i, (a, b) in enumerate(pairs)]

    def line_peer(step, other=0):
        return {"ep": lax.rem(z + step + CHIPS, CHIPS) * 2 + lax.rem(core + other, 2)}

    plane = [
        lax.rem(y + a, SIDE) * SIDE + lax.rem(x + b, SIDE) for a, b in plane_offsets()
    ]
    barrier = pltpu.get_barrier_semaphore()
    near = []
    for step in range(NEAR, 0, -1):
        for other in (0, 1):
            near += [line_peer(step, other), line_peer(-step, other)]
    near += [{"tp": j} for j in plane] + [line_peer(0, 1)]
    for peer in near:
        pl.semaphore_signal(barrier, inc=1, device_id=peer, device_id_type=MESH)
    for copy in loads:
        copy.start()

    def ready(*which):
        for i in which:
            loads[i].wait()

    ready(0, 1)
    values = resid_v[...].astype(F32)
    inverse = lax.rsqrt(jnp.mean(values * values, axis=-1, keepdims=True) + epsilon)
    mix = mix_v[...].astype(F32)
    normed = jnp.concatenate(
        [
            (values[:, j * 128 : (j + 1) * 128] * inverse * mix[j : j + 1, :]).astype(BF16)
            for j in range(WIDTH // 128)
        ],
        axis=1,
    )

    ready(2, 3, 4, 5, 6)
    queries = (dot(normed, wq[...]) * DK ** (-0.5)).astype(BF16).astype(F32)
    keys = dot(normed, wk[...]).astype(BF16).astype(F32)
    decay = dot(normed, wd[...]).astype(BF16).astype(F32)
    value_t = dot(wv[...], normed, ((1,), (1,))).astype(BF16).astype(F32)
    logit = decay + bias_v[pl.ds(head, 1), :]
    log_gate = jnp.minimum(logit, 0.0) - jnp.log(1.0 + jnp.exp(-jnp.abs(logit)))
    forget = jnp.exp(log_gate / gate_tau)

    ready(7)
    queries = queries.astype(BF16)
    row = lax.broadcasted_iota(jnp.int32, (SEQ, 2 * VC), 0)
    right = lax.broadcasted_iota(jnp.int32, (SEQ, 2 * VC), 1) // VC
    readout = jnp.zeros((SEQ, 2 * VC), F32)
    for t in range(0, SEQ, 2):
        two = []
        for u in (t, t + 1):
            new = (
                forget[u : u + 1, :] * state_v[u]
                + value_t[:, u : u + 1] * keys[u : u + 1, :]
            )
            state_out[u] = new
            two.append(new)
        new = jnp.concatenate(two, axis=0)
        high = new.astype(BF16)
        low = (new - high.astype(F32)).astype(BF16)
        read = dot(queries, high, ((1,), (1,))) + dot(queries, low, ((1,), (1,)))
        readout = jnp.where(row == t + right, read, readout)

    ready(8, 16)
    partial = dot(readout.astype(BF16), wp[...])
    for j in range(TPN):
        part_s[j] = partial[:, j * PART : (j + 1) * PART].astype(BF16)

    pl.semaphore_wait(barrier, len(near))
    for step in (NEAR, -NEAR):
        pl.semaphore_signal(near_sem.at[0], inc=1, device_id=line_peer(step), device_id_type=MESH)

    def send(src, dst, phase, peer):
        pltpu.make_async_remote_copy(
            src_ref=src,
            dst_ref=dst,
            send_sem=send_sem.at[phase],
            recv_sem=recv_sem.at[phase],
            device_id=peer,
            device_id_type=MESH,
        ).start()

    def settle(ref, sem, phase):
        rest = ref.at[pl.ds(0, ref.shape[0] - 1)]
        pltpu.make_async_copy(rest, rest, sem.at[phase]).wait()

    for j in plane:
        send(part_s.at[j], part_r.at[tp], 0, {"tp": j})
    part_r[pl.ds(tp, 1)] = part_s[pl.ds(tp, 1)]

    ready(9, 10, 11, 12)
    base = group_v[pl.ds(block, 1), :] * 4
    first = (base + pick_v[0:1, :]).astype(F32)
    second = (base + pick_v[1:2, :]).astype(F32)
    sub = lax.broadcasted_iota(jnp.int32, (8, PART), 0)
    packed = jnp.where(
        sub == 0,
        first,
        jnp.where(sub == 1, second, jnp.where(sub == 2, weight_v[0:1, :], weight_v[1:2, :])),
    )
    cols[...] = packed.T
    own = cols[pl.ds(pl.multiple_of(lax.rem(ep, PART // SEQ) * SEQ, SEQ), SEQ), :]
    lanes = lax.broadcasted_iota(jnp.int32, (SEQ, 2 * EXPERTS), 1)
    expert_lane = (lanes // 2).astype(F32)
    slot_lane = lax.rem(lanes, 2).astype(F32)
    pick_a = (own[:, 0:1] == expert_lane).astype(F32)
    pick_b = (own[:, 1:2] == expert_lane).astype(F32)
    below = (
        lax.broadcasted_iota(jnp.int32, (SEQ, SEQ), 1)
        < lax.broadcasted_iota(jnp.int32, (SEQ, SEQ), 0)
    ).astype(F32)
    both = pick_a + pick_b
    earlier = dot(below.astype(BF16), both.astype(BF16))
    here = (earlier == slot_lane).astype(F32)
    select = (both * here).astype(BF16)
    mixing = (own[:, 2:3] * pick_a + own[:, 3:4] * pick_b) * here
    mixing_out[...] = mixing
    select_t = select.astype(F32).T.astype(BF16)
    own_rows = resid_v[:, pl.ds(pl.multiple_of(tp * PART, PART), PART)].astype(F32)

    settle(part_r, recv_sem, 0)
    attention = jnp.sum(part_r[...].astype(F32), axis=0).astype(BF16)
    middle = (own_rows + attention.astype(F32)).astype(BF16)
    middle_out[...] = middle

    rows_s.reshape(2 * EXPERTS, PART)[...] = dot(select_t, middle).astype(BF16)
    pl.semaphore_wait(near_sem.at[0], 2)

    def to_line(src, dst, phase):
        for step in line_offsets():
            for other in (0, 1):
                if step == 0 and other == 0:
                    continue
                there = line_peer(step, other)
                send(src.at[there["ep"]], dst.at[ep], phase, there)
        dst[pl.ds(ep, 1)] = src[pl.ds(ep, 1)]

    to_line(rows_s, rows_r, 1)
    ready(13, 14, 15)
    gain = gain_v[...].astype(F32)
    settle(rows_r, recv_sem, 1)
    rows = rows_r.reshape(2 * EXPERTS, PART)[...].astype(F32)
    squares = jnp.sum(rows * rows, axis=1, keepdims=True)
    squares = jnp.broadcast_to(squares, (2 * EXPERTS, 128))
    squares_hi = squares.astype(BF16).astype(F32)
    squares_lo = squares - squares_hi
    scaled = (rows * gain).astype(BF16)
    gate_part = dot(scaled, wg[...])
    up_part = dot(scaled, wu[...])

    def owners(top, bottom):
        shape = (TPN, 8, top.shape[1])
        return jnp.concatenate([top.reshape(shape), bottom.reshape(shape)], axis=1).astype(BF16)

    hid_s[:, :, 0:FF] = owners(gate_part, up_part)
    hid_s[:, :, FF : FF + 128] = owners(squares_hi, squares_lo)
    for j in plane:
        send(hid_s.at[j], hid_r.at[tp], 2, {"tp": j})
    hid_r[pl.ds(tp, 1)] = hid_s[pl.ds(tp, 1)]
    settle(hid_r, recv_sem, 2)
    total = jnp.sum(hid_r[...].astype(F32), axis=0)
    square_sum = total[0:8, FF : FF + 128] + total[8:16, FF : FF + 128]
    scale = lax.rsqrt(square_sum / WIDTH + epsilon)
    scale = jnp.concatenate([scale, scale], axis=1)
    gate_pre = total[0:8, 0:FF] * scale
    up_pre = total[8:16, 0:FF] * scale
    active = gate_pre / (1.0 + jnp.exp(-gate_pre)) * up_pre
    act_s[...] = jnp.concatenate([active[:, 0:128], active[:, 128:256]], axis=0).astype(BF16)

    for j in plane:
        send(act_s, act_r.at[tp], 3, {"tp": j})
    act_r[pl.ds(tp, 1)] = act_s[...].reshape(1, 16, 128)
    settle(act_r, recv_sem, 3)
    acts = act_r[...].astype(F32)
    low = acts[:, 0:8, :].reshape(128, 128).astype(BF16)
    high = acts[:, 8:16, :].reshape(128, 128).astype(BF16)
    served = dot(low, wo[0:128, :]) + dot(high, wo[128:256, :])

    back_s.reshape(2 * EXPERTS, PART)[...] = served.astype(BF16)
    to_line(back_s, back_r, 4)
    settle(back_r, recv_sem, 4)
    back_out[...] = back_r.reshape(2 * EXPERTS, PART)[...]

    settle(part_s, send_sem, 0)
    settle(rows_s, send_sem, 1)
    settle(hid_s, send_sem, 2)
    settle(act_r, send_sem, 3)
    settle(back_s, send_sem, 4)


def output_kernel(middle, mixing, back, state, resid_out, state_out, out_v, sem):
    store = pltpu.make_async_copy(state, state_out, sem.at[0])
    store.start()
    mixing_hi = mixing[...].astype(BF16)
    mixing_lo = (mixing[...] - mixing_hi.astype(F32)).astype(BF16)
    mixture = dot(mixing_hi, back[...]) + dot(mixing_lo, back[...])
    out_v[...] = (middle[...].astype(F32) + mixture).astype(BF16)
    last = pltpu.make_async_copy(out_v, resid_out, sem.at[1])
    last.start()
    store.wait()
    last.wait()


def on_device(
    resid_in,
    state_in,
    mix_gain,
    query_weight,
    key_weight,
    decay_weight,
    value_weight,
    decay_bias,
    proj_weight,
    ffn_gain,
    expert_gate,
    expert_up,
    expert_down,
    route_group,
    route_pick,
    route_weight,
):
    args = (
        resid_in,
        state_in,
        mix_gain.reshape(WIDTH // 128, 128),
        query_weight,
        key_weight,
        decay_weight,
        value_weight.T,
        decay_bias.reshape(-1, DK),
        proj_weight,
        ffn_gain.reshape(1, PART),
        expert_gate,
        expert_up,
        expert_down,
        route_group.reshape(-1, 128),
        route_pick.T,
        route_weight.T,
    )
    vmem = pltpu.VMEM
    middle, mixing, back, state = pl.pallas_call(
        layer_kernel,
        out_shape=(
            pltpu.VMEM((SEQ, PART), BF16),
            pltpu.VMEM((SEQ, 2 * EXPERTS), F32),
            pltpu.VMEM((2 * EXPERTS, PART), BF16),
            pltpu.VMEM((SEQ, VC, DK), F32),
        ),
        in_specs=[pl.BlockSpec(memory_space=pl.ANY)] * len(args),
        out_specs=[pl.BlockSpec(memory_space=pltpu.VMEM)] * 4,
        scratch_shapes=[
            vmem((SEQ, WIDTH), BF16),
            vmem((WIDTH // 128, 128), BF16),
            vmem((WIDTH, DK), BF16),
            vmem((WIDTH, DK), BF16),
            vmem((WIDTH, DK), BF16),
            vmem((VC, WIDTH), BF16),
            vmem((4, DK), F32),
            vmem((2 * VC, WIDTH), BF16),
            vmem((1, PART), BF16),
            vmem((PART, FF), BF16),
            vmem((PART, FF), BF16),
            vmem((FF, PART), BF16),
            vmem((16, 128), jnp.int32),
            vmem((2, PART), jnp.int32),
            vmem((2, PART), F32),
            vmem((SEQ, VC, DK), F32),
            vmem((PART, 8), F32),
            vmem((TPN, SEQ, PART), BF16),
            vmem((TPN, SEQ, PART), BF16),
            vmem((EXPERTS, 2, PART), BF16),
            vmem((EXPERTS, 2, PART), BF16),
            vmem((TPN, 16, FF + 128), BF16),
            vmem((TPN, 16, FF + 128), BF16),
            vmem((16, 128), BF16),
            vmem((TPN, 16, 128), BF16),
            vmem((EXPERTS, 2, PART), BF16),
            vmem((EXPERTS, 2, PART), BF16),
            pltpu.SemaphoreType.DMA((17,)),
            pltpu.SemaphoreType.DMA((5,)),
            pltpu.SemaphoreType.DMA((5,)),
            pltpu.SemaphoreType.REGULAR((1,)),
        ],
        compiler_params=pltpu.CompilerParams(collective_id=0, has_side_effects=True),
    )(*args)
    return pl.pallas_call(
        output_kernel,
        out_shape=(
            jax.ShapeDtypeStruct((SEQ, PART), BF16),
            jax.ShapeDtypeStruct((SEQ, VC, DK), F32),
        ),
        in_specs=[pl.BlockSpec(memory_space=pltpu.VMEM)] * 4,
        out_specs=[pl.BlockSpec(memory_space=pl.ANY)] * 2,
        scratch_shapes=[vmem((SEQ, PART), BF16), pltpu.SemaphoreType.DMA((2,))],
        compiler_params=pltpu.CompilerParams(vmem_limit_bytes=4 << 20),
    )(*(pltpu.with_memory_space_constraint(a, pltpu.VMEM) for a in (middle, mixing, back, state)))


def solution(mesh):
    return jax.shard_map(
        on_device,
        mesh=mesh,
        in_specs=(
            P("ep", None),
            P("ep", "tp", None),
            P(),
            P(),
            P(),
            P(),
            P(None, "tp"),
            P(),
            P("tp", None),
            P("tp"),
            P("ep", "tp", None),
            P("ep", "tp", None),
            P("ep", None, "tp"),
            P(),
            P(),
            P(),
        ),
        out_specs=(P("ep", "tp"), P("ep", "tp", None)),
        check_vma=False,
    )
```

```python
import functools

import jax
import jax.numpy as jnp
from jax import lax
from jax.experimental import pallas as pl
from jax.experimental.pallas import tpu as pltpu
from jax.sharding import PartitionSpec as P

MESH = pl.DeviceIdType.MESH
F32 = jnp.float32
BF16 = jnp.bfloat16

epsilon = 1e-06
gate_tau = 16.0

SEQ = 32
WIDTH = 2048
DK = 128
DV = 256
VC = 64
PART = 128
FF = 256
CHIPS = 32
EXPERTS = 64
SIDE = 4
TPN = 16
NEAR = 8


def plane_offsets():
    steps = [(a, b) for a in range(SIDE) for b in range(SIDE) if a or b]
    return sorted(steps, key=lambda s: -(min(s[0], SIDE - s[0]) + min(s[1], SIDE - s[1])))


def line_offsets():
    return sorted(range(CHIPS), key=lambda s: -min(s, CHIPS - s))


def dot(a, b, dims=((1,), (0,))):
    return lax.dot_general(a, b, (dims, ((), ())), preferred_element_type=F32)


def layer_kernel(
    resid,
    state_in,
    mix_gain,
    query_w,
    key_w,
    decay_w,
    value_w,
    decay_bias,
    proj_w,
    ffn_gain,
    gate_w,
    up_w,
    down_w,
    group,
    pick,
    weight,
    middle_out,
    mixing_out,
    back_out,
    state_out,
    resid_v,
    mix_v,
    wq,
    wk,
    wd,
    wv,
    bias_v,
    wp,
    gain_v,
    wg,
    wu,
    wo,
    group_v,
    pick_v,
    weight_v,
    state_v,
    cols,
    part_s,
    part_r,
    rows_s,
    rows_r,
    hid_s,
    hid_r,
    back_s,
    back_r,
    load_sem,
    send_sem,
    recv_sem,
    near_sem,
):
    ep = lax.axis_index("ep")
    tp = lax.axis_index("tp")
    z = ep // 2
    core = lax.rem(ep, 2)
    y = tp // SIDE
    x = lax.rem(tp, SIDE)
    head = tp // (DV // VC)
    block = ep // (PART // SEQ)
    head_cols = pl.ds(pl.multiple_of(head * DK, DK), DK)
    block_cols = pl.ds(pl.multiple_of(block * PART, PART), PART)

    pairs = [
        (resid, resid_v),
        (mix_gain, mix_v),
        (query_w.at[:, head_cols], wq),
        (key_w.at[:, head_cols], wk),
        (decay_w.at[:, head_cols], wd),
        (value_w, wv),
        (decay_bias, bias_v),
        (state_in, state_v),
        (proj_w, wp.at[pl.ds(0, VC)]),
        (ffn_gain, gain_v),
        (group, group_v),
        (pick.at[:, block_cols], pick_v),
        (weight.at[:, block_cols], weight_v),
        (gate_w.at[0], wg),
        (up_w.at[0], wu),
        (down_w.at[0], wo.at[tp]),
        (proj_w, wp.at[pl.ds(VC, VC)]),
    ]
    loads = [pltpu.make_async_copy(a, b, load_sem.at[i]) for i, (a, b) in enumerate(pairs)]

    def line_peer(step, other=0):
        return {"ep": lax.rem(z + step + CHIPS, CHIPS) * 2 + lax.rem(core + other, 2)}

    plane = [
        lax.rem(y + a, SIDE) * SIDE + lax.rem(x + b, SIDE) for a, b in plane_offsets()
    ]
    barrier = pltpu.get_barrier_semaphore()
    near = []
    for step in range(NEAR, 0, -1):
        for other in (0, 1):
            near += [line_peer(step, other), line_peer(-step, other)]
    near += [{"tp": j} for j in plane] + [line_peer(0, 1)]
    for peer in near:
        pl.semaphore_signal(barrier, inc=1, device_id=peer, device_id_type=MESH)
    for copy in loads:
        copy.start()

    def ready(*which):
        for i in which:
            loads[i].wait()

    ready(0, 1)
    values = resid_v[...].astype(F32)
    inverse = lax.rsqrt(jnp.mean(values * values, axis=-1, keepdims=True) + epsilon)
    mix = mix_v[...].astype(F32)
    normed = jnp.concatenate(
        [
            (values[:, j * 128 : (j + 1) * 128] * inverse * mix[j : j + 1, :]).astype(BF16)
            for j in range(WIDTH // 128)
        ],
        axis=1,
    )

    ready(2, 3, 4, 5, 6)
    queries = (dot(normed, wq[...]) * DK ** (-0.5)).astype(BF16).astype(F32)
    keys = dot(normed, wk[...]).astype(BF16).astype(F32)
    decay = dot(normed, wd[...]).astype(BF16).astype(F32)
    value_t = dot(wv[...], normed, ((1,), (1,))).astype(BF16).astype(F32)
    logit = decay + bias_v[pl.ds(head, 1), :]
    log_gate = jnp.minimum(logit, 0.0) - jnp.log(1.0 + jnp.exp(-jnp.abs(logit)))
    forget = jnp.exp(log_gate / gate_tau)

    ready(7)
    queries = queries.astype(BF16)
    row = lax.broadcasted_iota(jnp.int32, (SEQ, 2 * VC), 0)
    right = lax.broadcasted_iota(jnp.int32, (SEQ, 2 * VC), 1) // VC
    readout = jnp.zeros((SEQ, 2 * VC), F32)
    for t in range(0, SEQ, 2):
        two = []
        for u in (t, t + 1):
            new = (
                forget[u : u + 1, :] * state_v[u]
                + value_t[:, u : u + 1] * keys[u : u + 1, :]
            )
            state_out[u] = new
            two.append(new)
        new = jnp.concatenate(two, axis=0)
        high = new.astype(BF16)
        low = (new - high.astype(F32)).astype(BF16)
        read = dot(queries, high, ((1,), (1,))) + dot(queries, low, ((1,), (1,)))
        readout = jnp.where(row == t + right, read, readout)

    ready(8, 16)
    partial = dot(readout.astype(BF16), wp[...])
    for j in range(TPN):
        part_s[j] = partial[:, j * PART : (j + 1) * PART].astype(BF16)

    pl.semaphore_wait(barrier, len(near))
    for step in (NEAR, -NEAR):
        pl.semaphore_signal(near_sem.at[0], inc=1, device_id=line_peer(step), device_id_type=MESH)

    def send(src, dst, phase, peer):
        pltpu.make_async_remote_copy(
            src_ref=src,
            dst_ref=dst,
            send_sem=send_sem.at[phase],
            recv_sem=recv_sem.at[phase],
            device_id=peer,
            device_id_type=MESH,
        ).start()

    def settle(ref, sem, phase, count=None):
        rest = ref.at[pl.ds(0, ref.shape[0] - 1 if count is None else count)]
        pltpu.make_async_copy(rest, rest, sem.at[phase]).wait()

    for j in plane:
        send(part_s.at[j], part_r.at[tp], 0, {"tp": j})
    part_r[pl.ds(tp, 1)] = part_s[pl.ds(tp, 1)]

    ready(15)
    for j in reversed(plane):
        send(wo.at[tp], wo.at[tp], 3, {"tp": j})

    ready(9, 10, 11, 12)
    base = group_v[pl.ds(block, 1), :] * 4
    first = (base + pick_v[0:1, :]).astype(F32)
    second = (base + pick_v[1:2, :]).astype(F32)
    sub = lax.broadcasted_iota(jnp.int32, (8, PART), 0)
    packed = jnp.where(
        sub == 0,
        first,
        jnp.where(sub == 1, second, jnp.where(sub == 2, weight_v[0:1, :], weight_v[1:2, :])),
    )
    cols[...] = packed.T
    own = cols[pl.ds(pl.multiple_of(lax.rem(ep, PART // SEQ) * SEQ, SEQ), SEQ), :]
    lanes = lax.broadcasted_iota(jnp.int32, (SEQ, 2 * EXPERTS), 1)
    expert_lane = (lanes // 2).astype(F32)
    slot_lane = lax.rem(lanes, 2).astype(F32)
    pick_a = (own[:, 0:1] == expert_lane).astype(F32)
    pick_b = (own[:, 1:2] == expert_lane).astype(F32)
    below = (
        lax.broadcasted_iota(jnp.int32, (SEQ, SEQ), 1)
        < lax.broadcasted_iota(jnp.int32, (SEQ, SEQ), 0)
    ).astype(F32)
    both = pick_a + pick_b
    earlier = dot(below.astype(BF16), both.astype(BF16))
    here = (earlier == slot_lane).astype(F32)
    select = (both * here).astype(BF16)
    mixing = (own[:, 2:3] * pick_a + own[:, 3:4] * pick_b) * here
    mixing_out[...] = mixing
    select_t = select.astype(F32).T.astype(BF16)
    own_rows = resid_v[:, pl.ds(pl.multiple_of(tp * PART, PART), PART)].astype(F32)

    settle(part_r, recv_sem, 0)
    attention = jnp.sum(part_r[...].astype(F32), axis=0).astype(BF16)
    middle = (own_rows + attention.astype(F32)).astype(BF16)
    middle_out[...] = middle

    rows_s.reshape(2 * EXPERTS, PART)[...] = dot(select_t, middle).astype(BF16)
    pl.semaphore_wait(near_sem.at[0], 2)

    def to_line(src, dst, phase):
        for step in line_offsets():
            for other in (0, 1):
                if step == 0 and other == 0:
                    continue
                there = line_peer(step, other)
                send(src.at[there["ep"]], dst.at[ep], phase, there)
        dst[pl.ds(ep, 1)] = src[pl.ds(ep, 1)]

    to_line(rows_s, rows_r, 1)

    ready(13, 14)
    gain = gain_v[...].astype(F32)
    settle(rows_r, recv_sem, 1)
    rows = rows_r.reshape(2 * EXPERTS, PART)[...].astype(F32)
    squares = jnp.sum(rows * rows, axis=1, keepdims=True)
    squares = jnp.broadcast_to(squares, (2 * EXPERTS, 128))
    squares_hi = squares.astype(BF16).astype(F32)
    squares_lo = squares - squares_hi
    scaled = (rows * gain).astype(BF16)
    gate_part = dot(scaled, wg[...])
    up_part = dot(scaled, wu[...])

    def owners(top, bottom):
        shape = (TPN, 8, top.shape[1])
        return jnp.concatenate([top.reshape(shape), bottom.reshape(shape)], axis=1).astype(BF16)

    hid_s[:, :, 0:FF] = owners(gate_part, up_part)
    hid_s[:, :, FF : FF + 128] = owners(squares_hi, squares_lo)
    for j in plane:
        send(hid_s.at[j], hid_r.at[tp], 2, {"tp": j})
    hid_r[pl.ds(tp, 1)] = hid_s[pl.ds(tp, 1)]
    settle(hid_r, recv_sem, 2)
    total = jnp.sum(hid_r[...].astype(F32), axis=0)
    square_sum = total[0:8, FF : FF + 128] + total[8:16, FF : FF + 128]
    scale = lax.rsqrt(square_sum / WIDTH + epsilon)
    scale = jnp.concatenate([scale, scale], axis=1)
    gate_pre = total[0:8, 0:FF] * scale
    up_pre = total[8:16, 0:FF] * scale
    active = gate_pre / (1.0 + jnp.exp(-gate_pre)) * up_pre
    active = active.astype(BF16)

    settle(wo, recv_sem, 3)
    for j in range(TPN):
        served = dot(active, wo[j])
        back_s[4 * j : 4 * j + 4] = served.astype(BF16).reshape(4, 2, PART)

    def give_back(j, b):
        there = {"ep": tp * 4 + b, "tp": j}
        send(back_s.at[j * 4 + b], back_r.at[ep], 4, there)

    for j in plane:
        for b in range(4):
            give_back(j, b)
    for b in range(4):
        pl.when(tp * 4 + b != ep)(functools.partial(give_back, tp, b))
    own_block = ep // 4 == tp

    @pl.when(own_block)
    def _():
        back_r[pl.ds(ep, 1)] = back_s[pl.ds(ep, 1)]

    def both_ends(sem):
        pl.when(own_block)(lambda: settle(back_r, sem, 4, EXPERTS - 1))
        pl.when(jnp.logical_not(own_block))(lambda: settle(back_r, sem, 4, EXPERTS))

    both_ends(recv_sem)
    back_out[...] = back_r.reshape(2 * EXPERTS, PART)[...]

    settle(part_s, send_sem, 0)
    settle(rows_s, send_sem, 1)
    settle(hid_s, send_sem, 2)
    settle(wo, send_sem, 3)
    both_ends(send_sem)


def output_kernel(middle, mixing, back, state, resid_out, state_out, out_v, sem):
    store = pltpu.make_async_copy(state, state_out, sem.at[0])
    store.start()
    mixing_hi = mixing[...].astype(BF16)
    mixing_lo = (mixing[...] - mixing_hi.astype(F32)).astype(BF16)
    mixture = dot(mixing_hi, back[...]) + dot(mixing_lo, back[...])
    out_v[...] = (middle[...].astype(F32) + mixture).astype(BF16)
    last = pltpu.make_async_copy(out_v, resid_out, sem.at[1])
    last.start()
    store.wait()
    last.wait()


def on_device(
    resid_in,
    state_in,
    mix_gain,
    query_weight,
    key_weight,
    decay_weight,
    value_weight,
    decay_bias,
    proj_weight,
    ffn_gain,
    expert_gate,
    expert_up,
    expert_down,
    route_group,
    route_pick,
    route_weight,
):
    args = (
        resid_in,
        state_in,
        mix_gain.reshape(WIDTH // 128, 128),
        query_weight,
        key_weight,
        decay_weight,
        value_weight.T,
        decay_bias.reshape(-1, DK),
        proj_weight,
        ffn_gain.reshape(1, PART),
        expert_gate,
        expert_up,
        expert_down,
        route_group.reshape(-1, 128),
        route_pick.T,
        route_weight.T,
    )
    vmem = pltpu.VMEM
    middle, mixing, back, state = pl.pallas_call(
        layer_kernel,
        out_shape=(
            pltpu.VMEM((SEQ, PART), BF16),
            pltpu.VMEM((SEQ, 2 * EXPERTS), F32),
            pltpu.VMEM((2 * EXPERTS, PART), BF16),
            pltpu.VMEM((SEQ, VC, DK), F32),
        ),
        in_specs=[pl.BlockSpec(memory_space=pl.ANY)] * len(args),
        out_specs=[pl.BlockSpec(memory_space=pltpu.VMEM)] * 4,
        scratch_shapes=[
            vmem((SEQ, WIDTH), BF16),
            vmem((WIDTH // 128, 128), BF16),
            vmem((WIDTH, DK), BF16),
            vmem((WIDTH, DK), BF16),
            vmem((WIDTH, DK), BF16),
            vmem((VC, WIDTH), BF16),
            vmem((4, DK), F32),
            vmem((2 * VC, WIDTH), BF16),
            vmem((1, PART), BF16),
            vmem((PART, FF), BF16),
            vmem((PART, FF), BF16),
            vmem((TPN, FF, PART), BF16),
            vmem((16, 128), jnp.int32),
            vmem((2, PART), jnp.int32),
            vmem((2, PART), F32),
            vmem((SEQ, VC, DK), F32),
            vmem((PART, 8), F32),
            vmem((TPN, SEQ, PART), BF16),
            vmem((TPN, SEQ, PART), BF16),
            vmem((EXPERTS, 2, PART), BF16),
            vmem((EXPERTS, 2, PART), BF16),
            vmem((TPN, 16, FF + 128), BF16),
            vmem((TPN, 16, FF + 128), BF16),
            vmem((EXPERTS, 2, PART), BF16),
            vmem((EXPERTS, 2, PART), BF16),
            pltpu.SemaphoreType.DMA((17,)),
            pltpu.SemaphoreType.DMA((5,)),
            pltpu.SemaphoreType.DMA((5,)),
            pltpu.SemaphoreType.REGULAR((1,)),
        ],
        compiler_params=pltpu.CompilerParams(collective_id=0, has_side_effects=True),
    )(*args)
    return pl.pallas_call(
        output_kernel,
        out_shape=(
            jax.ShapeDtypeStruct((SEQ, PART), BF16),
            jax.ShapeDtypeStruct((SEQ, VC, DK), F32),
        ),
        in_specs=[pl.BlockSpec(memory_space=pltpu.VMEM)] * 4,
        out_specs=[pl.BlockSpec(memory_space=pl.ANY)] * 2,
        scratch_shapes=[vmem((SEQ, PART), BF16), pltpu.SemaphoreType.DMA((2,))],
        compiler_params=pltpu.CompilerParams(vmem_limit_bytes=4 << 20),
    )(*(pltpu.with_memory_space_constraint(a, pltpu.VMEM) for a in (middle, mixing, back, state)))


def solution(mesh):
    return jax.shard_map(
        on_device,
        mesh=mesh,
        in_specs=(
            P("ep", None),
            P("ep", "tp", None),
            P(),
            P(),
            P(),
            P(),
            P(None, "tp"),
            P(),
            P("tp", None),
            P("tp"),
            P("ep", "tp", None),
            P("ep", "tp", None),
            P("ep", None, "tp"),
            P(),
            P(),
            P(),
        ),
        out_specs=(P("ep", "tp"), P("ep", "tp", None)),
        check_vma=False,
    )
```

```python
import functools

import jax
import jax.numpy as jnp
from jax import lax
from jax.experimental import pallas as pl
from jax.experimental.pallas import tpu as pltpu
from jax.sharding import PartitionSpec as P

MESH = pl.DeviceIdType.MESH
F32 = jnp.float32
BF16 = jnp.bfloat16

epsilon = 1e-06
gate_tau = 16.0

SEQ = 32
WIDTH = 2048
DK = 128
DV = 256
VC = 64
PART = 128
FF = 256
CHIPS = 32
EXPERTS = 64
SIDE = 4
TPN = 16
NEAR = 8


def plane_offsets():
    steps = [(a, b) for a in range(SIDE) for b in range(SIDE) if a or b]
    return sorted(steps, key=lambda s: -(min(s[0], SIDE - s[0]) + min(s[1], SIDE - s[1])))


def line_offsets():
    return sorted(range(CHIPS), key=lambda s: -min(s, CHIPS - s))


def dot(a, b, dims=((1,), (0,))):
    return lax.dot_general(a, b, (dims, ((), ())), preferred_element_type=F32)


def layer_kernel(
    resid,
    state_in,
    mix_gain,
    query_w,
    key_w,
    decay_w,
    value_w,
    decay_bias,
    proj_w,
    ffn_gain,
    gate_w,
    up_w,
    down_w,
    group,
    pick,
    weight,
    middle_out,
    mixing_out,
    back_out,
    state_out,
    resid_v,
    mix_v,
    wq,
    wk,
    wd,
    wv,
    bias_v,
    wp,
    gain_v,
    wg,
    wu,
    wo,
    group_v,
    pick_v,
    weight_v,
    state_v,
    cols,
    part_s,
    part_r,
    rows_s,
    rows_r,
    hid_s,
    hid_r,
    sq_s,
    sq_r,
    back_s,
    back_r,
    load_sem,
    send_sem,
    recv_sem,
    near_sem,
):
    ep = lax.axis_index("ep")
    tp = lax.axis_index("tp")
    z = ep // 2
    core = lax.rem(ep, 2)
    y = tp // SIDE
    x = lax.rem(tp, SIDE)
    head = tp // (DV // VC)
    block = ep // (PART // SEQ)
    head_cols = pl.ds(pl.multiple_of(head * DK, DK), DK)
    block_cols = pl.ds(pl.multiple_of(block * PART, PART), PART)

    pairs = [
        (resid, resid_v),
        (mix_gain, mix_v),
        (query_w.at[:, head_cols], wq),
        (key_w.at[:, head_cols], wk),
        (decay_w.at[:, head_cols], wd),
        (value_w, wv),
        (decay_bias, bias_v),
        (state_in, state_v),
        (proj_w, wp.at[pl.ds(0, VC)]),
        (ffn_gain, gain_v),
        (group, group_v),
        (pick.at[:, block_cols], pick_v),
        (weight.at[:, block_cols], weight_v),
        (gate_w.at[0], wg),
        (up_w.at[0], wu),
        (down_w.at[0], wo.at[tp]),
        (proj_w, wp.at[pl.ds(VC, VC)]),
    ]
    loads = [pltpu.make_async_copy(a, b, load_sem.at[i]) for i, (a, b) in enumerate(pairs)]

    def line_peer(step, other=0):
        return {"ep": lax.rem(z + step + CHIPS, CHIPS) * 2 + lax.rem(core + other, 2)}

    plane = [
        lax.rem(y + a, SIDE) * SIDE + lax.rem(x + b, SIDE) for a, b in plane_offsets()
    ]
    barrier = pltpu.get_barrier_semaphore()
    near = []
    for step in range(NEAR, 0, -1):
        for other in (0, 1):
            near += [line_peer(step, other), line_peer(-step, other)]
    near += [{"tp": j} for j in plane] + [line_peer(0, 1)]
    for peer in near:
        pl.semaphore_signal(barrier, inc=1, device_id=peer, device_id_type=MESH)
    for copy in loads:
        copy.start()

    def ready(*which):
        for i in which:
            loads[i].wait()

    ready(0, 1)
    values = resid_v[...].astype(F32)
    inverse = lax.rsqrt(jnp.mean(values * values, axis=-1, keepdims=True) + epsilon)
    mix = mix_v[...].astype(F32)
    normed = jnp.concatenate(
        [
            (values[:, j * 128 : (j + 1) * 128] * inverse * mix[j : j + 1, :]).astype(BF16)
            for j in range(WIDTH // 128)
        ],
        axis=1,
    )

    ready(2, 3, 4, 5, 6)
    queries = (dot(normed, wq[...]) * DK ** (-0.5)).astype(BF16).astype(F32)
    keys = dot(normed, wk[...]).astype(BF16).astype(F32)
    decay = dot(normed, wd[...]).astype(BF16).astype(F32)
    value_t = dot(wv[...], normed, ((1,), (1,))).astype(BF16).astype(F32)
    logit = decay + bias_v[pl.ds(head, 1), :]
    log_gate = jnp.minimum(logit, 0.0) - jnp.log(1.0 + jnp.exp(-jnp.abs(logit)))
    forget = jnp.exp(log_gate / gate_tau)

    ready(7)
    queries = queries.astype(BF16)
    row = lax.broadcasted_iota(jnp.int32, (SEQ, 2 * VC), 0)
    right = lax.broadcasted_iota(jnp.int32, (SEQ, 2 * VC), 1) // VC
    readout = jnp.zeros((SEQ, 2 * VC), F32)
    for t in range(0, SEQ, 2):
        two = []
        for u in (t, t + 1):
            new = (
                forget[u : u + 1, :] * state_v[u]
                + value_t[:, u : u + 1] * keys[u : u + 1, :]
            )
            state_out[u] = new
            two.append(new)
        new = jnp.concatenate(two, axis=0)
        high = new.astype(BF16)
        low = (new - high.astype(F32)).astype(BF16)
        read = dot(queries, high, ((1,), (1,))) + dot(queries, low, ((1,), (1,)))
        readout = jnp.where(row == t + right, read, readout)

    ready(8, 16)
    partial = dot(readout.astype(BF16), wp[...])
    for j in range(TPN):
        part_s[j] = partial[:, j * PART : (j + 1) * PART].astype(BF16)

    pl.semaphore_wait(barrier, len(near))
    for step in (NEAR, -NEAR):
        pl.semaphore_signal(near_sem.at[0], inc=1, device_id=line_peer(step), device_id_type=MESH)

    def send(src, dst, phase, peer):
        pltpu.make_async_remote_copy(
            src_ref=src,
            dst_ref=dst,
            send_sem=send_sem.at[phase],
            recv_sem=recv_sem.at[phase],
            device_id=peer,
            device_id_type=MESH,
        ).start()

    def settle(ref, sem, phase, count=None):
        rest = ref.at[pl.ds(0, ref.shape[0] - 1 if count is None else count)]
        pltpu.make_async_copy(rest, rest, sem.at[phase]).wait()

    for j in plane:
        send(part_s.at[j], part_r.at[tp], 0, {"tp": j})
    part_r[pl.ds(tp, 1)] = part_s[pl.ds(tp, 1)]

    ready(15)
    for j in reversed(plane):
        send(wo.at[tp], wo.at[tp], 3, {"tp": j})

    ready(9, 10, 11, 12)
    base = group_v[pl.ds(block, 1), :] * 4
    first = (base + pick_v[0:1, :]).astype(F32)
    second = (base + pick_v[1:2, :]).astype(F32)
    sub = lax.broadcasted_iota(jnp.int32, (8, PART), 0)
    packed = jnp.where(
        sub == 0,
        first,
        jnp.where(sub == 1, second, jnp.where(sub == 2, weight_v[0:1, :], weight_v[1:2, :])),
    )
    cols[...] = packed.T
    own = cols[pl.ds(pl.multiple_of(lax.rem(ep, PART // SEQ) * SEQ, SEQ), SEQ), :]
    lanes = lax.broadcasted_iota(jnp.int32, (SEQ, 2 * EXPERTS), 1)
    expert_lane = (lanes // 2).astype(F32)
    slot_lane = lax.rem(lanes, 2).astype(F32)
    pick_a = (own[:, 0:1] == expert_lane).astype(F32)
    pick_b = (own[:, 1:2] == expert_lane).astype(F32)
    below = (
        lax.broadcasted_iota(jnp.int32, (SEQ, SEQ), 1)
        < lax.broadcasted_iota(jnp.int32, (SEQ, SEQ), 0)
    ).astype(F32)
    both = pick_a + pick_b
    earlier = dot(below.astype(BF16), both.astype(BF16))
    here = (earlier == slot_lane).astype(F32)
    select = (both * here).astype(BF16)
    mixing = (own[:, 2:3] * pick_a + own[:, 3:4] * pick_b) * here
    mixing_out[...] = mixing
    select_t = select.astype(F32).T.astype(BF16)
    own_rows = resid_v[:, pl.ds(pl.multiple_of(tp * PART, PART), PART)].astype(F32)

    settle(part_r, recv_sem, 0)
    attention = jnp.sum(part_r[...].astype(F32), axis=0).astype(BF16)
    middle = (own_rows + attention.astype(F32)).astype(BF16)
    middle_out[...] = middle

    rows_s.reshape(2 * EXPERTS, PART)[...] = dot(select_t, middle).astype(BF16)
    pl.semaphore_wait(near_sem.at[0], 2)

    def to_line(src, dst, phase):
        for step in line_offsets():
            for other in (0, 1):
                if step == 0 and other == 0:
                    continue
                there = line_peer(step, other)
                send(src.at[there["ep"]], dst.at[ep], phase, there)
        dst[pl.ds(ep, 1)] = src[pl.ds(ep, 1)]

    to_line(rows_s, rows_r, 1)

    ready(13, 14)
    gain = gain_v[...].astype(F32)
    settle(rows_r, recv_sem, 1)
    rows = rows_r.reshape(2 * EXPERTS, PART)[...].astype(F32)
    squares = jnp.sum(rows * rows, axis=1, keepdims=True)
    sq_s[...] = jnp.broadcast_to(squares, (2 * EXPERTS, 128)).T[0:1, :]
    scaled = (rows * gain).astype(BF16)
    gate_part = dot(scaled, wg[...])
    up_part = dot(scaled, wu[...])

    def owners(top, bottom):
        shape = (TPN, 8, top.shape[1])
        return jnp.concatenate([top.reshape(shape), bottom.reshape(shape)], axis=1).astype(BF16)

    hid_s[...] = owners(gate_part, up_part)
    for j in plane:
        send(sq_s, sq_r.at[tp], 5, {"tp": j})
        send(hid_s.at[j], hid_r.at[tp], 2, {"tp": j})
    sq_r[pl.ds(tp, 1)] = sq_s[...].reshape(1, 1, 128)
    hid_r[pl.ds(tp, 1)] = hid_s[pl.ds(tp, 1)]
    settle(hid_r, recv_sem, 2)
    total = jnp.sum(hid_r[...].astype(F32), axis=0)
    settle(sq_r, recv_sem, 5)
    square_row = jnp.sum(sq_r[...], axis=0)
    own_lane = lax.broadcasted_iota(jnp.int32, (8, 128), 1) == (
        tp * 8 + lax.broadcasted_iota(jnp.int32, (8, 128), 0)
    )
    square_sum = jnp.sum(jnp.where(own_lane, square_row, 0.0), axis=1, keepdims=True)
    scale = lax.rsqrt(square_sum / WIDTH + epsilon)
    gate_pre = total[0:8, 0:FF] * scale
    up_pre = total[8:16, 0:FF] * scale
    active = gate_pre / (1.0 + jnp.exp(-gate_pre)) * up_pre
    active = active.astype(BF16)

    settle(wo, recv_sem, 3)
    for j in range(TPN):
        served = dot(active, wo[j])
        back_s[4 * j : 4 * j + 4] = served.astype(BF16).reshape(4, 2, PART)

    def give_back(j, b):
        there = {"ep": tp * 4 + b, "tp": j}
        send(back_s.at[j * 4 + b], back_r.at[ep], 4, there)

    for j in plane:
        for b in range(4):
            give_back(j, b)
    for b in range(4):
        pl.when(tp * 4 + b != ep)(functools.partial(give_back, tp, b))
    own_block = ep // 4 == tp

    @pl.when(own_block)
    def _():
        back_r[pl.ds(ep, 1)] = back_s[pl.ds(ep, 1)]

    def both_ends(sem):
        pl.when(own_block)(lambda: settle(back_r, sem, 4, EXPERTS - 1))
        pl.when(jnp.logical_not(own_block))(lambda: settle(back_r, sem, 4, EXPERTS))

    both_ends(recv_sem)
    back_out[...] = back_r.reshape(2 * EXPERTS, PART)[...]

    settle(part_s, send_sem, 0)
    settle(rows_s, send_sem, 1)
    settle(hid_s, send_sem, 2)
    settle(sq_r, send_sem, 5)
    settle(wo, send_sem, 3)
    both_ends(send_sem)


def output_kernel(middle, mixing, back, state, resid_out, state_out, out_v, sem):
    store = pltpu.make_async_copy(state, state_out, sem.at[0])
    store.start()
    mixing_hi = mixing[...].astype(BF16)
    mixing_lo = (mixing[...] - mixing_hi.astype(F32)).astype(BF16)
    mixture = dot(mixing_hi, back[...]) + dot(mixing_lo, back[...])
    out_v[...] = (middle[...].astype(F32) + mixture).astype(BF16)
    last = pltpu.make_async_copy(out_v, resid_out, sem.at[1])
    last.start()
    store.wait()
    last.wait()


def on_device(
    resid_in,
    state_in,
    mix_gain,
    query_weight,
    key_weight,
    decay_weight,
    value_weight,
    decay_bias,
    proj_weight,
    ffn_gain,
    expert_gate,
    expert_up,
    expert_down,
    route_group,
    route_pick,
    route_weight,
):
    args = (
        resid_in,
        state_in,
        mix_gain.reshape(WIDTH // 128, 128),
        query_weight,
        key_weight,
        decay_weight,
        value_weight.T,
        decay_bias.reshape(-1, DK),
        proj_weight,
        ffn_gain.reshape(1, PART),
        expert_gate,
        expert_up,
        expert_down,
        route_group.reshape(-1, 128),
        route_pick.T,
        route_weight.T,
    )
    vmem = pltpu.VMEM
    middle, mixing, back, state = pl.pallas_call(
        layer_kernel,
        out_shape=(
            pltpu.VMEM((SEQ, PART), BF16),
            pltpu.VMEM((SEQ, 2 * EXPERTS), F32),
            pltpu.VMEM((2 * EXPERTS, PART), BF16),
            pltpu.VMEM((SEQ, VC, DK), F32),
        ),
        in_specs=[pl.BlockSpec(memory_space=pl.ANY)] * len(args),
        out_specs=[pl.BlockSpec(memory_space=pltpu.VMEM)] * 4,
        scratch_shapes=[
            vmem((SEQ, WIDTH), BF16),
            vmem((WIDTH // 128, 128), BF16),
            vmem((WIDTH, DK), BF16),
            vmem((WIDTH, DK), BF16),
            vmem((WIDTH, DK), BF16),
            vmem((VC, WIDTH), BF16),
            vmem((4, DK), F32),
            vmem((2 * VC, WIDTH), BF16),
            vmem((1, PART), BF16),
            vmem((PART, FF), BF16),
            vmem((PART, FF), BF16),
            vmem((TPN, FF, PART), BF16),
            vmem((16, 128), jnp.int32),
            vmem((2, PART), jnp.int32),
            vmem((2, PART), F32),
            vmem((SEQ, VC, DK), F32),
            vmem((PART, 8), F32),
            vmem((TPN, SEQ, PART), BF16),
            vmem((TPN, SEQ, PART), BF16),
            vmem((EXPERTS, 2, PART), BF16),
            vmem((EXPERTS, 2, PART), BF16),
            vmem((TPN, 16, FF), BF16),
            vmem((TPN, 16, FF), BF16),
            vmem((1, 128), F32),
            vmem((TPN, 1, 128), F32),
            vmem((EXPERTS, 2, PART), BF16),
            vmem((EXPERTS, 2, PART), BF16),
            pltpu.SemaphoreType.DMA((17,)),
            pltpu.SemaphoreType.DMA((6,)),
            pltpu.SemaphoreType.DMA((6,)),
            pltpu.SemaphoreType.REGULAR((1,)),
        ],
        compiler_params=pltpu.CompilerParams(collective_id=0, has_side_effects=True),
    )(*args)
    return pl.pallas_call(
        output_kernel,
        out_shape=(
            jax.ShapeDtypeStruct((SEQ, PART), BF16),
            jax.ShapeDtypeStruct((SEQ, VC, DK), F32),
        ),
        in_specs=[pl.BlockSpec(memory_space=pltpu.VMEM)] * 4,
        out_specs=[pl.BlockSpec(memory_space=pl.ANY)] * 2,
        scratch_shapes=[vmem((SEQ, PART), BF16), pltpu.SemaphoreType.DMA((2,))],
        compiler_params=pltpu.CompilerParams(vmem_limit_bytes=4 << 20),
    )(*(pltpu.with_memory_space_constraint(a, pltpu.VMEM) for a in (middle, mixing, back, state)))


def solution(mesh):
    return jax.shard_map(
        on_device,
        mesh=mesh,
        in_specs=(
            P("ep", None),
            P("ep", "tp", None),
            P(),
            P(),
            P(),
            P(),
            P(None, "tp"),
            P(),
            P("tp", None),
            P("tp"),
            P("ep", "tp", None),
            P("ep", "tp", None),
            P("ep", None, "tp"),
            P(),
            P(),
            P(),
        ),
        out_specs=(P("ep", "tp"), P("ep", "tp", None)),
        check_vma=False,
    )
```
